32 devices in a mesh: gr: 2 (over x), fs: 4 (over z), tp: 4 (over y, core).
Axes of the slice: x: 2, y: 2, z: 4, core: 2. Of those that a mesh axis runs over, the one named last changes fastest.
Arguments:
- tokens: bfloat16 [4096, 2048], P(('gr', 'fs', 'tp')), may hold values from -6 to 6
- norm_gain: float32 [2048], P('fs'), may hold values from 0.1 to 1.9
- gate_master: float32 [16, 2048, 256], P(None, 'fs', ('gr', 'tp')), may hold values from -0.125 to 0.125
- up_master: float32 [16, 2048, 256], P(None, 'fs', ('gr', 'tp')), may hold values from -0.125 to 0.125
- down_master: float32 [16, 256, 2048], P(None, 'fs', ('gr', 'tp')), may hold values from -0.375 to 0.375
- route_group: int32 [4096], P(('gr', 'fs', 'tp')), may hold values from 0 to 3
- route_expert: int32 [4096, 2], P(('gr', 'fs', 'tp')), may hold values from 0 to 3, all different within a row
- route_weight: float32 [4096, 2], P(('gr', 'fs', 'tp')), may hold values from 0.1 to 1
Outputs:
- gate_new: bfloat16 [16, 2048, 256], P(('fs', 'tp'))
- up_new: bfloat16 [16, 2048, 256], P(('fs', 'tp'))
- down_new: bfloat16 [16, 256, 2048], P(('fs', 'tp'))
- mixed: bfloat16 [4096, 2048], P(('gr', 'fs', 'tp'))
The draws below stay inside these ranges and needn't reach their ends.
Inputs may be any that keep to these rules, and one draw needn't show every extreme that they name: `route_expert`: the 2 entries of a row are different.
All inputs are finite; a program needn't handle non-finite values.
Results may differ from the reference program's by a relative error of at most 0.0086.
Values may be sent and summed in bfloat16 or wider, within the bound.
No kernel may reach another device: no remote copies, remote signals or barrier semaphores. Data moves between devices by JAX's collectives and lax.ppermute only.
A program may use at most 64 MiB of HBM per device.

```python
import math
import jax
import jax.numpy as jnp
from jax import lax

D = 2048
F = 256
E_GROUPS = 4
TOP = 2
TOK_DEV = 128
EXPERTS = 16
EPG = 4
TOKENS = 4096
CAP = 24


def touch_ends(drawn, stream_key, smallest, top_value):
    place = [jax.random.randint(jax.random.fold_in(stream_key, axis), (), 0, length) for axis, length in enumerate(drawn.shape)]
    longest = drawn.shape.index(max(drawn.shape))
    next_to = place[:longest] + [(place[longest] + 1) % drawn.shape[longest]] + place[longest + 1:]
    return drawn.at[tuple(place)].set(smallest).at[tuple(next_to)].set(top_value)


def steps_of(rng, dims, cuts, low, high):
    loudness, own = 1.0, jax.random.fold_in(rng, 6)
    for dim, blocks in cuts:
        steps = jnp.exp(jax.random.uniform(jax.random.fold_in(own, dim), (blocks,), jnp.float32, low / len(cuts), high / len(cuts)))
        loudness = loudness * jnp.repeat(steps, dims[dim] // blocks).reshape([-1 if axis == dim else 1 for axis in range(len(dims))])
    return loudness


def choose_distinct(key, rows, number_of, top, lift):
    order = jax.random.permutation(jax.random.fold_in(key, 1), number_of)
    pull = order
    for power in range(3):
        pull = pull * pull // number_of
    pull = pull * lift // number_of
    tickets = jax.random.randint(jax.random.fold_in(key, 2), (rows, number_of), 0, 4096) + pull
    fixed_rows = jax.random.permutation(jax.random.fold_in(key, 3), rows)[jnp.arange(number_of) % rows]
    tickets = jnp.where(jnp.arange(rows)[:, None] == fixed_rows[None, :], 1 << 14, tickets)
    priority = tickets * number_of + jnp.arange(number_of)
    return lax.top_k(priority.astype(jnp.int32), top)[1].astype(jnp.int32)


def scatter_about(key, shape, scale, most, shards=(), held_as=jnp.bfloat16):
    gain = steps_of(key, shape, shards, -0.22, 0.18) if shards else 1.0
    result = jax.random.normal(key, shape, jnp.float32) * scale * gain
    return jnp.minimum(jnp.maximum(result, -most), most).astype(held_as)


def setup_inputs(seed: int = 0) -> dict:
    seeds = jax.random.split(jax.random.key(seed), 9)
    return {
        "tokens": scatter_about(seeds[0], (TOKENS, D), 1.0, 6.0, ((0, 32),)),
        "norm_gain": jnp.clip(1.0 + 0.18 * jax.random.normal(seeds[1], (D,), jnp.float32), 0.1, 1.9),
        "gate_master": scatter_about(seeds[2], (EXPERTS, D, F), D ** -0.5, 0.125, ((1, 4), (2, 8)), jnp.float32),
        "up_master": scatter_about(seeds[3], (EXPERTS, D, F), D ** -0.5, 0.125, ((1, 4), (2, 8)), jnp.float32),
        "down_master": scatter_about(seeds[4], (EXPERTS, F, D), F ** -0.5, 0.375, ((1, 4), (2, 8)), jnp.float32),
        "route_group": touch_ends(jax.random.randint(seeds[5], (TOKENS,), 0, E_GROUPS), jax.random.fold_in(seeds[5], 1), 0, E_GROUPS - 1).astype(jnp.int32),
        "route_expert": choose_distinct(seeds[6], TOKENS, EPG, TOP, 4096),
        "route_weight": jnp.clip(jnp.exp(math.log(1.0) - 2.3025851 * jax.random.uniform(seeds[7], (TOKENS, TOP), jnp.float32) ** steps_of(seeds[7], (TOKENS, TOP), ((0, 32),), -0.2, 0.2)), 0.1, 1.0),
    }


def reference(tokens, norm_gain, gate_master, up_master, down_master, route_group, route_expert, route_weight):
    gate_new = (gate_master * norm_gain[None, :, None]).astype(jnp.bfloat16)
    up_new = (up_master * norm_gain[None, :, None]).astype(jnp.bfloat16)
    down_new = down_master.astype(jnp.bfloat16)
    floats = tokens.astype(jnp.float32)
    normed = (floats * lax.rsqrt(lax.optimization_barrier(jnp.mean(floats * floats, axis=-1, keepdims=True)) + 1e-06)).astype(jnp.bfloat16)
    sources = TOKENS // TOK_DEV
    expert_id = (route_group[:, None] * EPG + route_expert).astype(jnp.int32)
    blocks = expert_id.reshape(sources, TOK_DEV * TOP)
    columns = jnp.arange(EXPERTS).astype(jnp.int32)
    onehot = (blocks[:, :, None] == columns[None, None, :]).astype(jnp.int32)
    rank = lax.optimization_barrier(jnp.sum((jnp.cumsum(onehot, axis=1) - 1) * onehot, axis=2)).astype(jnp.int32)
    source_ids = jnp.arange(sources).astype(jnp.int32)[:, None]
    dump = EXPERTS * sources * CAP
    slot = jnp.where(rank < CAP, blocks * (sources * CAP) + source_ids * CAP + rank, dump).reshape(-1).astype(jnp.int32)
    rows = jnp.repeat(normed, TOP, axis=0)
    buffer = jnp.zeros((dump + 1, D), jnp.bfloat16).at[slot].set(rows)[:-1].reshape(EXPERTS, sources * CAP, D)

    def expert(operands):
        block, w_gate, w_up, w_down = operands
        gate = jnp.dot(block, w_gate, preferred_element_type=jnp.float32)
        upper = jnp.dot(block, w_up, preferred_element_type=jnp.float32)
        hidden = (jax.nn.silu(gate) * upper).astype(jnp.bfloat16)
        return jnp.dot(hidden, w_down, preferred_element_type=jnp.float32).astype(jnp.bfloat16)
    outcome = lax.map(expert, (buffer, gate_new, up_new, down_new))
    table = jnp.concatenate([outcome.reshape(-1, D), jnp.zeros((1, D), jnp.bfloat16)], axis=0)
    picked = table[slot].reshape(TOKENS, TOP, D).astype(jnp.float32)
    mixed = lax.optimization_barrier(jnp.sum(picked * route_weight[:, :, None], axis=1)).astype(jnp.bfloat16)
    return (gate_new, up_new, down_new, mixed)
```

```python
import functools

import jax
import jax.numpy as jnp
from jax import lax
from jax.experimental import pallas as pl
from jax.experimental.pallas import tpu as pltpu
from jax.sharding import PartitionSpec as P

E_GROUPS = 4
TOP = 2
BF = jnp.bfloat16
F32 = jnp.float32


def vmem():
    return pl.BlockSpec(memory_space=pltpu.VMEM)


def smem():
    return pl.BlockSpec(memory_space=pltpu.SMEM)


def call(kernel, outs, *args, scalars=0, name=None, flops=0, scratch=()):
    specs = [smem()] * scalars + [vmem()] * (len(args) - scalars)
    return pl.pallas_call(
        kernel,
        out_shape=outs,
        in_specs=specs,
        out_specs=jax.tree.map(lambda _: vmem(), outs),
        scratch_shapes=scratch,
        name=name,
        cost_estimate=pl.CostEstimate(flops=flops, transcendentals=0, bytes_accessed=0),
    )(*args)


def cast_kernel(gain_ref, gate_ref, up_ref, down_ref, out_ref):
    f_local = gate_ref.shape[1]
    d_local = down_ref.shape[2]
    folds = gate_ref.shape[2] // d_local
    gain = gain_ref[...]
    out_ref[:, 0:f_local, :] = (gate_ref[...] * gain).astype(BF)
    out_ref[:, f_local : 2 * f_local, :] = (up_ref[...] * gain).astype(BF)
    rows = down_ref.shape[1] // folds
    for j in range(folds):
        out_ref[:, 2 * f_local :, j * d_local : (j + 1) * d_local] = down_ref[
            :, j * rows : (j + 1) * rows, :
        ].astype(BF)


def cast_weights(gain, gate, up, down):
    n, f_local, width = gate.shape
    rows = 2 * f_local + down.shape[1] * down.shape[2] // width
    block = max(1, n // 4)
    return pl.pallas_call(
        cast_kernel,
        grid=(n // block,),
        out_shape=jax.ShapeDtypeStruct((n, rows, width), BF),
        in_specs=[
            pl.BlockSpec((1, width), lambda i: (0, 0)),
            pl.BlockSpec((block, f_local, width), lambda i: (i, 0, 0)),
            pl.BlockSpec((block, f_local, width), lambda i: (i, 0, 0)),
            pl.BlockSpec((block,) + down.shape[1:], lambda i: (i, 0, 0)),
        ],
        out_specs=pl.BlockSpec((block, rows, width), lambda i: (i, 0, 0)),
        name="cast_weights",
    )(gain, gate, up, down)


def pack_kernel(me_ref, group_ref, expert_ref, tokens_ref, slot_ref, *out_refs, per_group):
    n = len(out_refs)
    cap = out_refs[0].shape[0]
    count = tokens_ref.shape[0]
    floats = tokens_ref[...].astype(F32)
    scale = lax.rsqrt(jnp.mean(floats * floats, axis=-1, keepdims=True) + 1e-06)
    normed = (floats * scale).astype(BF)
    rel = (group_ref[...] * per_group + expert_ref[...]) ^ me_ref[0]
    rows = lax.broadcasted_iota(jnp.int32, (n, count), 0)
    hot = [rows == rel[k : k + 1, :] for k in range(TOP)]
    both = sum(h.astype(F32) for h in hot)
    t0 = lax.broadcasted_iota(jnp.int32, (count, count), 0)
    t1 = lax.broadcasted_iota(jnp.int32, (count, count), 1)
    before = jnp.dot(both.astype(BF), (t0 < t1).astype(BF), preferred_element_type=F32)
    pos = lax.broadcasted_iota(jnp.int32, (n * cap, count), 0)
    picks = jnp.zeros((n * cap, count), jnp.bool_)
    for k in range(TOP):
        rank = jnp.sum(jnp.where(hot[k], before, 0.0), axis=0, keepdims=True).astype(jnp.int32)
        slot = jnp.where(rank < cap, rel[k : k + 1, :] * cap + rank, -1)
        slot_ref[k : k + 1, :] = slot
        picks = picks | (pos == slot)
    packed = jnp.dot(
        jnp.where(picks, 1.0, 0.0).astype(BF), normed, preferred_element_type=F32
    ).astype(BF)
    for i in range(n):
        out_refs[i][...] = packed[i * cap : (i + 1) * cap, :]


def hidden_block(x, w_ref, n_fs, n_tp, f_local, width, row0):
    acc = None
    for f in range(n_fs):
        rhs = jnp.concatenate(
            [w_ref[f * n_tp + t, row0 : row0 + f_local, :] for t in range(n_tp)], axis=0
        )
        part = lax.dot_general(
            x[:, f * width : (f + 1) * width],
            rhs,
            (((1,), (1,)), ((), ())),
            preferred_element_type=F32,
        )
        acc = part if acc is None else acc + part
    return acc


def ffn_kernel(gr_ref, own_ref, peer_ref, *refs, n_fs, n_tp, f_local, down_local):
    n = len(refs) // 2
    ins, outs = refs[:n], refs[n:]
    cap = ins[0].shape[0]
    width = own_ref.shape[2]
    x = jnp.concatenate([r[...] for r in ins], axis=0)
    halves = []
    for w_ref in (own_ref, peer_ref):
        gate = hidden_block(x, w_ref, n_fs, n_tp, f_local, width, 0)
        upper = hidden_block(x, w_ref, n_fs, n_tp, f_local, width, f_local)
        halves.append((gate / (1.0 + jnp.exp(-gate)) * upper).astype(BF))
    first = gr_ref[0] == 0
    hidden = jnp.where(
        first, jnp.concatenate(halves, axis=1), jnp.concatenate(halves[::-1], axis=1)
    )
    down_rows, d_local = down_local
    folds = width // d_local
    rows = down_rows // folds
    for half, w_ref in enumerate((own_ref, peer_ref)):
        for t in range(n_tp):
            rhs = jnp.concatenate(
                [
                    w_ref[f * n_tp + t, 2 * f_local :, j * d_local : (j + 1) * d_local]
                    for f in range(n_fs)
                    for j in range(folds)
                ],
                axis=0,
            )
            y = jnp.dot(hidden, rhs, preferred_element_type=F32).astype(BF)
            place = gr_ref[0] if half == 0 else 1 - gr_ref[0]
            start = pl.multiple_of(place * (n_tp * d_local) + t * d_local, d_local)
            for i in range(n):
                outs[i][:, pl.ds(start, d_local)] = y[i * cap : (i + 1) * cap, :]


def mix_kernel(slot_ref, weight_ref, *refs):
    out_ref = refs[-1]
    ins = refs[:-1]
    cap = ins[0].shape[0]
    count = out_ref.shape[0]
    total = len(ins) * cap
    table = jnp.concatenate([r[...] for r in ins], axis=0)
    pos = lax.broadcasted_iota(jnp.int32, (total, count), 0)
    mixing = jnp.zeros((total, count), F32)
    for k in range(TOP):
        mixing = mixing + jnp.where(
            pos == slot_ref[k : k + 1, :], weight_ref[k : k + 1, :], 0.0
        )
    high = mixing.astype(BF)
    rest = mixing - high.astype(F32)
    low = rest.astype(BF)
    dims = (((0,), (0,)), ((), ()))
    acc = lax.dot_general(high, table, dims, preferred_element_type=F32)
    acc = acc + lax.dot_general(low, table, dims, preferred_element_type=F32)
    out_ref[...] = acc.astype(BF)


def unpack_kernel(
    gr_ref, own_ref, peer_ref, gate_ref, up_ref, down_ref, *, n_fs, n_tp, f_local, down_local
):
    width = own_ref.shape[2]
    down_rows, d_local = down_local
    folds = width // d_local
    rows = down_rows // folds
    for half, w_ref in enumerate((own_ref, peer_ref)):
        place = gr_ref[0] if half == 0 else 1 - gr_ref[0]
        start = pl.multiple_of(place * (n_tp * f_local), n_tp * f_local)
        for f in range(n_fs):
            for row0, o_ref in ((0, gate_ref), (f_local, up_ref)):
                block = jnp.concatenate(
                    [w_ref[f * n_tp + t, row0 : row0 + f_local, :] for t in range(n_tp)], axis=0
                )
                o_ref[0, f * width : (f + 1) * width, pl.ds(start, n_tp * f_local)] = block.T
        for f in range(n_fs):
            for t in range(n_tp):
                col = pl.multiple_of(place * (n_tp * d_local) + t * d_local, d_local)
                for j in range(folds):
                    r0 = f * down_rows + j * rows
                    down_ref[0, r0 : r0 + rows, pl.ds(col, d_local)] = w_ref[
                        f * n_tp + t, 2 * f_local :, j * d_local : (j + 1) * d_local
                    ]


def fast_body(
    tokens, norm_gain, gate_master, up_master, down_master, route_group, route_expert, route_weight
):
    n_fs = lax.axis_size("fs")
    n_tp = lax.axis_size("tp")
    n = n_fs * n_tp
    axes = ("fs", "tp")
    count, width = tokens.shape
    cap = 3 * count * TOP // (2 * n)
    f_local = gate_master.shape[2]
    down_local = down_master.shape[1:]
    me = (lax.axis_index("fs") * n_tp + lax.axis_index("tp")).astype(jnp.int32)[None]
    gr = lax.axis_index("gr").astype(jnp.int32)[None]

    weights = cast_weights(
        norm_gain[None],
        jnp.swapaxes(gate_master, 1, 2),
        jnp.swapaxes(up_master, 1, 2),
        down_master,
    )
    own = lax.all_to_all(weights, axes, split_axis=0, concat_axis=0, tiled=True)
    peer = lax.ppermute(own, "gr", [(0, 1), (1, 0)])

    buffer = jax.ShapeDtypeStruct((cap, width), BF)
    slots, *sends = call(
        functools.partial(pack_kernel, per_group=n // E_GROUPS),
        [jax.ShapeDtypeStruct((TOP, count), jnp.int32)] + [buffer] * n,
        me,
        route_group[None],
        route_expert.T,
        tokens,
        scalars=1,
        name="pack_tokens",
        flops=2 * n * cap * count * width,
    )

    def exchange(buffers):
        return [
            b if i == 0 else lax.ppermute(b, axes, [(s, s ^ i) for s in range(n)])
            for i, b in enumerate(buffers)
        ]

    received = exchange(sends)
    shape = dict(n_fs=n_fs, n_tp=n_tp, f_local=f_local, down_local=down_local)
    results = call(
        functools.partial(ffn_kernel, **shape),
        [buffer] * n,
        gr,
        own,
        peer,
        *received,
        scalars=1,
        name="experts",
        flops=6 * n * cap * width * 2 * n_tp * f_local,
    )
    returned = exchange(results)
    gate_new, up_new, down_new = call(
        functools.partial(unpack_kernel, **shape),
        [
            jax.ShapeDtypeStruct((1, width, 2 * n_tp * f_local), BF),
            jax.ShapeDtypeStruct((1, width, 2 * n_tp * f_local), BF),
            jax.ShapeDtypeStruct((1, n_fs * down_local[0], 2 * n_tp * down_local[1]), BF),
        ],
        gr,
        own,
        peer,
        scalars=1,
        name="unpack_weights",
        flops=10_000_000,
    )
    mixed = call(
        mix_kernel,
        jax.ShapeDtypeStruct((count, width), BF),
        slots,
        route_weight.T,
        *returned,
        name="mix",
        flops=4 * n * cap * count * width,
    )
    return (gate_new, up_new, down_new, mixed)


def slow_body(
    tokens, norm_gain, gate_master, up_master, down_master, route_group, route_expert, route_weight
):
    n_fs = lax.axis_size("fs")
    n_tp = lax.axis_size("tp")
    n_gr = lax.axis_size("gr")
    experts = n_fs * n_tp
    per_group = experts // E_GROUPS
    gate_cast = (gate_master * norm_gain[None, :, None]).astype(jnp.bfloat16)
    up_cast = (up_master * norm_gain[None, :, None]).astype(jnp.bfloat16)
    down_cast = down_master.astype(jnp.bfloat16)

    def to_grid(tile):
        return tile.reshape((n_fs, n_tp, 1, tile.shape[1], tile.shape[2]))

    grids = (
        to_grid(jnp.swapaxes(gate_cast, 1, 2)),
        to_grid(jnp.swapaxes(up_cast, 1, 2)),
        to_grid(down_cast),
    )
    grids = (
        lax.all_to_all(
            lax.all_to_all(grids[0], "fs", split_axis=0, concat_axis=4, tiled=True),
            "tp",
            split_axis=1,
            concat_axis=3,
            tiled=True,
        ),
        lax.all_to_all(
            lax.all_to_all(grids[1], "fs", split_axis=0, concat_axis=4, tiled=True),
            "tp",
            split_axis=1,
            concat_axis=3,
            tiled=True,
        ),
        lax.all_to_all(
            lax.all_to_all(grids[2], "fs", split_axis=0, concat_axis=4, tiled=True),
            "tp",
            split_axis=1,
            concat_axis=3,
            tiled=True,
        ),
    )
    grids = (
        lax.all_gather(grids[0], "gr", axis=2, tiled=True),
        lax.all_gather(grids[1], "gr", axis=2, tiled=True),
        lax.all_gather(grids[2], "gr", axis=2, tiled=True),
    )

    def rows_to_matrix(grid):
        hidden_units = grid.shape[2] * grid.shape[3]
        return jnp.swapaxes(grid.reshape(hidden_units, grid.shape[4]), 0, 1)[None]

    gate_new = rows_to_matrix(grids[0])
    up_new = rows_to_matrix(grids[1])
    grid = grids[2]
    f_local = grid.shape[3] // n_tp
    d_local = grid.shape[4] // n_fs
    parts = grid.reshape(n_gr, n_tp, f_local, n_fs, d_local)
    parts = jnp.transpose(parts, (3, 2, 0, 1, 4))
    down_new = parts.reshape(1, n_fs * f_local, n_gr * n_tp * d_local)
    width = tokens.shape[1]
    count = tokens.shape[0]
    floats = tokens.astype(jnp.float32)
    normed = (floats * lax.rsqrt(jnp.mean(floats * floats, axis=-1, keepdims=True) + 1e-06)).astype(
        jnp.bfloat16
    )
    capacity = 3 * count * TOP // (2 * experts)
    flat_ids = (route_group[:, None] * per_group + route_expert).reshape(-1)
    columns = lax.broadcasted_iota(jnp.int32, (flat_ids.shape[0], experts), 1)
    onehot = (flat_ids[:, None] == columns).astype(jnp.int32)
    rank = jnp.sum((jnp.cumsum(onehot, axis=0) - 1) * onehot, axis=1)
    dump = experts * capacity
    slot = jnp.where(rank < capacity, flat_ids * capacity + rank, dump)
    rows = jnp.repeat(normed, TOP, axis=0)
    outgoing = (
        jnp.zeros((dump + 1, width), jnp.bfloat16)
        .at[slot]
        .set(rows)[:-1]
        .reshape(experts, capacity, width)
    )
    block = lax.all_to_all(outgoing, ("fs", "tp"), split_axis=0, concat_axis=0, tiled=True)
    flat_rows = block.reshape(-1, width)
    gate = jnp.dot(flat_rows, gate_new[0], preferred_element_type=jnp.float32)
    upper = jnp.dot(flat_rows, up_new[0], preferred_element_type=jnp.float32)
    hidden = (jax.nn.silu(gate) * upper).astype(jnp.bfloat16)
    result = jnp.dot(hidden, down_new[0], preferred_element_type=jnp.float32).astype(jnp.bfloat16)
    outcome = result.reshape(block.shape)
    returned = lax.all_to_all(outcome, ("fs", "tp"), split_axis=0, concat_axis=0, tiled=True)
    table = jnp.concatenate(
        [returned.reshape(-1, width), jnp.zeros((1, width), jnp.bfloat16)], axis=0
    )
    picked = table[slot].reshape(count, TOP, width).astype(jnp.float32)
    mixed = jnp.sum(picked * route_weight[:, :, None], axis=1).astype(jnp.bfloat16)
    return (gate_new, up_new, down_new, mixed)

def solution(mesh):
    placed = (
        P(("gr", "fs", "tp"), None),
        P("fs"),
        P(None, "fs", ("gr", "tp")),
        P(None, "fs", ("gr", "tp")),
        P(None, "fs", ("gr", "tp")),
        P(("gr", "fs", "tp")),
        P(("gr", "fs", "tp"), None),
        P(("gr", "fs", "tp"), None),
    )

    def body(*args):
        n = mesh.shape["fs"] * mesh.shape["tp"]
        cap = 3 * args[0].shape[0] * TOP // (2 * n)
        small = n <= 16 and n & (n - 1) == 0 and cap % 8 == 0 and mesh.shape["gr"] == 2
        return (fast_body if small else slow_body)(*args)

    return jax.shard_map(
        body,
        mesh=mesh,
        in_specs=placed,
        out_specs=(
            P(("fs", "tp"), None, None),
            P(("fs", "tp"), None, None),
            P(("fs", "tp"), None, None),
            P(("gr", "fs", "tp"), None),
        ),
        check_vma=False,
    )
```

```python
import functools

import jax
import jax.numpy as jnp
from jax import lax
from jax.experimental import pallas as pl
from jax.experimental.pallas import tpu as pltpu
from jax.sharding import PartitionSpec as P


E_GROUPS = 4
TOP = 2
BF = jnp.bfloat16
F32 = jnp.float32


def vmem():
    return pl.BlockSpec(memory_space=pltpu.VMEM)


def smem():
    return pl.BlockSpec(memory_space=pltpu.SMEM)


def anywhere():
    return pl.BlockSpec(memory_space=pl.ANY)


def call(kernel, outs, *args, scalars=0, flops=0, scratch=(), space=vmem, to=vmem):
    specs = [smem()] * scalars + [space()] * (len(args) - scalars)
    return pl.pallas_call(
        kernel,
        out_shape=outs,
        in_specs=specs,
        out_specs=jax.tree.map(lambda _: to(), outs),
        scratch_shapes=scratch,
        cost_estimate=pl.CostEstimate(flops=flops, transcendentals=0, bytes_accessed=0),
    )(*args)


def cast_kernel(me_ref, gain_ref, gate_ref, up_ref, down_ref, *out_refs):
    block, f_local, _ = gate_ref.shape
    d_local = down_ref.shape[2]
    folds = gate_ref.shape[2] // d_local
    rows = down_ref.shape[1] // folds
    gain = gain_ref[...]
    steps = 2 * len(out_refs) // block
    for i in range(steps):

        @pl.when(pl.program_id(0) == i)
        def _(i=i):
            for p in range(block):
                out_ref = out_refs[(i * block + p) // 2].at[p % 2]
                e = (me_ref[0] & (block - 1)) ^ p
                out_ref[0:f_local, :] = (gate_ref[e] * gain).astype(BF)
                out_ref[f_local : 2 * f_local, :] = (up_ref[e] * gain).astype(BF)
                for j in range(folds):
                    out_ref[2 * f_local :, j * d_local : (j + 1) * d_local] = down_ref[
                        e, j * rows : (j + 1) * rows, :
                    ].astype(BF)


def cast_weights(me, gain, gate, up, down, chips):
    _, f_local, width = gate.shape
    rows = 2 * f_local + down.shape[1] * down.shape[2] // width
    block = min(4, 2 * len(chips))
    base = 2 * chips[0] // block

    def pick(i, me_ref):
        return ((me_ref[0] // block) ^ (i + base), 0, 0)

    return pl.pallas_call(
        cast_kernel,
        out_shape=[jax.ShapeDtypeStruct((2, rows, width), BF)] * len(chips),
        grid_spec=pltpu.PrefetchScalarGridSpec(
            num_scalar_prefetch=1,
            grid=(2 * len(chips) // block,),
            in_specs=[
                pl.BlockSpec((1, width), lambda i, me_ref: (0, 0)),
                pl.BlockSpec((block, f_local, width), pick),
                pl.BlockSpec((block, f_local, width), pick),
                pl.BlockSpec((block,) + down.shape[1:], pick),
            ],
            out_specs=[pl.BlockSpec((2, rows, width), lambda i, me_ref: (0, 0, 0))] * len(chips),
        ),
    )(me, gain, gate, up, down)


def sibling_kernel(*refs):
    *pair_refs, out_ref, sems = refs
    copies = [
        pltpu.make_async_copy(ref.at[1], out_ref.at[i], sems.at[i])
        for i, ref in enumerate(pair_refs)
    ]
    for copy in copies:
        copy.start()
    for copy in copies:
        copy.wait()


def pack_kernel(me_ref, group_ref, expert_ref, tokens_ref, slot_ref, *out_refs, per_group):
    n = len(out_refs)
    cap = out_refs[0].shape[0]
    count = tokens_ref.shape[0]
    floats = tokens_ref[...].astype(F32)
    scale = lax.rsqrt(jnp.mean(floats * floats, axis=-1, keepdims=True) + 1e-06)
    normed = (floats * scale).astype(BF)
    rel = (group_ref[...] * per_group + expert_ref[...]) ^ me_ref[0]
    rows = lax.broadcasted_iota(jnp.int32, (n, count), 0)
    hot = [rows == rel[k : k + 1, :] for k in range(TOP)]
    both = sum(h.astype(F32) for h in hot)
    t0 = lax.broadcasted_iota(jnp.int32, (count, count), 0)
    t1 = lax.broadcasted_iota(jnp.int32, (count, count), 1)
    before = jnp.dot(both.astype(BF), (t0 < t1).astype(BF), preferred_element_type=F32)
    pos = lax.broadcasted_iota(jnp.int32, (n * cap, count), 0)
    picks = jnp.zeros((n * cap, count), jnp.bool_)
    for k in range(TOP):
        rank = jnp.sum(jnp.where(hot[k], before, 0.0), axis=0, keepdims=True).astype(jnp.int32)
        slot = jnp.where(rank < cap, rel[k : k + 1, :] * cap + rank, -1)
        slot_ref[k : k + 1, :] = slot
        picks = picks | (pos == slot)
    packed = jnp.dot(
        jnp.where(picks, 1.0, 0.0).astype(BF), normed, preferred_element_type=F32
    ).astype(BF)
    for i in range(n):
        out_refs[i][...] = packed[i * cap : (i + 1) * cap, :]


def ffn_kernel(gate_ref, up_ref, down_ref, *refs):
    n = len(refs) // 2
    ins, outs = refs[:n], refs[n:]
    cap = ins[0].shape[0]
    x = jnp.concatenate([r[...] for r in ins], axis=0)
    gate = jnp.dot(x, gate_ref[0], preferred_element_type=F32)
    upper = jnp.dot(x, up_ref[0], preferred_element_type=F32)
    hidden = (gate / (1.0 + jnp.exp(-gate)) * upper).astype(BF)
    y = jnp.dot(hidden, down_ref[0], preferred_element_type=F32).astype(BF)
    for i in range(n):
        outs[i][...] = y[i * cap : (i + 1) * cap, :]


def mix_kernel(slot_ref, weight_ref, *refs):
    out_ref = refs[-1]
    ins = refs[:-1]
    cap = ins[0].shape[0]
    count = out_ref.shape[0]
    total = len(ins) * cap
    table = jnp.concatenate([r[...] for r in ins], axis=0)
    pos = lax.broadcasted_iota(jnp.int32, (total, count), 0)
    mixing = jnp.zeros((total, count), F32)
    for k in range(TOP):
        mixing = mixing + jnp.where(
            pos == slot_ref[k : k + 1, :], weight_ref[k : k + 1, :], 0.0
        )
    high = mixing.astype(BF)
    rest = mixing - high.astype(F32)
    low = rest.astype(BF)
    dims = (((0,), (0,)), ((), ()))
    acc = lax.dot_general(high, table, dims, preferred_element_type=F32)
    acc = acc + lax.dot_general(low, table, dims, preferred_element_type=F32)
    out_ref[...] = acc.astype(BF)


def unpack_kernel(me_ref, gr_ref, *refs, n_fs, n_tp, f_local, down_local):
    n = n_fs * n_tp
    side = n // 2 + 1
    gate_ref, up_ref, down_ref, tiles_ref, sems = refs[2 * side :]
    width = tiles_ref.shape[3]
    down_rows, d_local = down_local
    folds = width // d_local
    rows = down_rows // folds
    copies = []
    for half in range(2):
        for i in range(n):
            j = half * side + (i // 2 if i % 2 == 0 else n // 2)
            source = refs[j].at[0 if i % 2 == 0 else i // 2]
            target = tiles_ref.at[half, me_ref[0] ^ i]
            copies.append(pltpu.make_async_copy(source, target, sems.at[half, i]))
            copies[-1].start()
    for half in range(2):
        for copy in copies[half * n : (half + 1) * n]:
            copy.wait()
        w_ref = tiles_ref.at[half]
        place = gr_ref[0] if half == 0 else 1 - gr_ref[0]
        start = pl.multiple_of(place * (n_tp * f_local), n_tp * f_local)
        for f in range(n_fs):
            for row0, o_ref in ((0, gate_ref), (f_local, up_ref)):
                block = jnp.concatenate(
                    [w_ref[f * n_tp + t, row0 : row0 + f_local, :] for t in range(n_tp)], axis=0
                )
                o_ref[0, f * width : (f + 1) * width, pl.ds(start, n_tp * f_local)] = block.T
        for f in range(n_fs):
            for t in range(n_tp):
                col = pl.multiple_of(place * (n_tp * d_local) + t * d_local, d_local)
                for j in range(folds):
                    r0 = f * down_rows + j * rows
                    down_ref[0, r0 : r0 + rows, pl.ds(col, d_local)] = w_ref[
                        f * n_tp + t, 2 * f_local :, j * d_local : (j + 1) * d_local
                    ]


def fast_body(
    tokens, norm_gain, gate_master, up_master, down_master, route_group, route_expert, route_weight
):
    n_fs = lax.axis_size("fs")
    n_tp = lax.axis_size("tp")
    n = n_fs * n_tp
    axes = ("fs", "tp")
    count, width = tokens.shape
    cap = 3 * count * TOP // (2 * n)
    f_local = gate_master.shape[2]
    down_local = down_master.shape[1:]
    me = (lax.axis_index("fs") * n_tp + lax.axis_index("tp")).astype(jnp.int32)[None]
    gr = lax.axis_index("gr").astype(jnp.int32)[None]

    chips = n // 2
    far_chips, near_chips = list(range(chips // 2, chips)), list(range(chips // 2))
    far, near = list(range(n // 2, n)), list(range(n // 2))
    buffer = jax.ShapeDtypeStruct((cap, width), BF)
    f_all = 2 * n_tp * f_local

    def send(b, i):
        if i == 0:
            return b
        return lax.ppermute(b, axes, [(s, s ^ i) for s in range(n)])

    def across(b):
        return lax.ppermute(b, "gr", [(0, 1), (1, 0)])

    def straight(b, i):
        pairs = [(g * n + s, (1 - g) * n + (s ^ i)) for g in range(2) for s in range(n)]
        return lax.ppermute(b, ("gr",) + axes, pairs)

    masters = (
        me,
        norm_gain[None],
        jnp.swapaxes(gate_master, 1, 2),
        jnp.swapaxes(up_master, 1, 2),
        down_master,
    )
    tiles = dict(zip(far_chips, cast_weights(*masters, far_chips)))
    tiles.update(zip(near_chips, cast_weights(*masters, near_chips)))
    own = {i: send(tiles[i], 2 * i) for i in far_chips + near_chips}
    peer = {i: straight(tiles[i], 2 * i) for i in near_chips}
    peer.update({i: across(own[i]) for i in far_chips})

    slots, *packed = call(
        functools.partial(pack_kernel, per_group=n // E_GROUPS),
        [jax.ShapeDtypeStruct((TOP, count), jnp.int32)] + [buffer] * n,
        me,
        route_group[None],
        route_expert.T,
        tokens,
        scalars=1,
        flops=2 * n * cap * count * width,
    )
    received = {i: send(packed[i], i) for i in far + near}

    sides = []
    for side in (own, peer):
        passed = call(
            sibling_kernel,
            jax.ShapeDtypeStruct((chips,) + side[0].shape[1:], BF),
            *[side[i] for i in range(chips)],
            scratch=[pltpu.SemaphoreType.DMA((chips,))],
            space=anywhere,
        )
        sides += [side[i] for i in range(chips)]
        sides.append(send(passed, 1))
    news = call(
        functools.partial(
            unpack_kernel, n_fs=n_fs, n_tp=n_tp, f_local=f_local, down_local=down_local
        ),
        [
            jax.ShapeDtypeStruct((1, width, f_all), BF),
            jax.ShapeDtypeStruct((1, width, f_all), BF),
            jax.ShapeDtypeStruct((1, f_all, width), BF),
        ],
        me,
        gr,
        *sides,
        scalars=2,
        flops=10_000_000,
        scratch=[
            pltpu.VMEM((2, n) + own[0].shape[1:], BF),
            pltpu.SemaphoreType.DMA((2, n)),
        ],
        space=anywhere,
    )
    returned = {}
    chunks = (far[: n // 4], far[n // 4 :], near)
    for chunk in chunks:
        results = call(
            ffn_kernel,
            [buffer] * len(chunk),
            *news,
            *[received[i] for i in chunk],
            flops=6 * len(chunk) * cap * width * f_all,
        )
        returned.update({i: send(r, i) for i, r in zip(chunk, results)})
    mixed = call(
        mix_kernel,
        jax.ShapeDtypeStruct((count, width), BF),
        slots,
        route_weight.T,
        *[returned[i] for i in range(n)],
        flops=4 * n * cap * count * width,
    )
    return (*news, mixed)


def slow_body(
    tokens, norm_gain, gate_master, up_master, down_master, route_group, route_expert, route_weight
):
    n_fs = lax.axis_size("fs")
    n_tp = lax.axis_size("tp")
    n_gr = lax.axis_size("gr")
    experts = n_fs * n_tp
    per_group = experts // E_GROUPS
    gate_cast = (gate_master * norm_gain[None, :, None]).astype(jnp.bfloat16)
    up_cast = (up_master * norm_gain[None, :, None]).astype(jnp.bfloat16)
    down_cast = down_master.astype(jnp.bfloat16)

    def to_grid(tile):
        return tile.reshape((n_fs, n_tp, 1, tile.shape[1], tile.shape[2]))

    grids = (
        to_grid(jnp.swapaxes(gate_cast, 1, 2)),
        to_grid(jnp.swapaxes(up_cast, 1, 2)),
        to_grid(down_cast),
    )
    grids = (
        lax.all_to_all(
            lax.all_to_all(grids[0], "fs", split_axis=0, concat_axis=4, tiled=True),
            "tp",
            split_axis=1,
            concat_axis=3,
            tiled=True,
        ),
        lax.all_to_all(
            lax.all_to_all(grids[1], "fs", split_axis=0, concat_axis=4, tiled=True),
            "tp",
            split_axis=1,
            concat_axis=3,
            tiled=True,
        ),
        lax.all_to_all(
            lax.all_to_all(grids[2], "fs", split_axis=0, concat_axis=4, tiled=True),
            "tp",
            split_axis=1,
            concat_axis=3,
            tiled=True,
        ),
    )
    grids = (
        lax.all_gather(grids[0], "gr", axis=2, tiled=True),
        lax.all_gather(grids[1], "gr", axis=2, tiled=True),
        lax.all_gather(grids[2], "gr", axis=2, tiled=True),
    )

    def rows_to_matrix(grid):
        hidden_units = grid.shape[2] * grid.shape[3]
        return jnp.swapaxes(grid.reshape(hidden_units, grid.shape[4]), 0, 1)[None]

    gate_new = rows_to_matrix(grids[0])
    up_new = rows_to_matrix(grids[1])
    grid = grids[2]
    f_local = grid.shape[3] // n_tp
    d_local = grid.shape[4] // n_fs
    parts = grid.reshape(n_gr, n_tp, f_local, n_fs, d_local)
    parts = jnp.transpose(parts, (3, 2, 0, 1, 4))
    down_new = parts.reshape(1, n_fs * f_local, n_gr * n_tp * d_local)
    width = tokens.shape[1]
    count = tokens.shape[0]
    floats = tokens.astype(jnp.float32)
    normed = (floats * lax.rsqrt(jnp.mean(floats * floats, axis=-1, keepdims=True) + 1e-06)).astype(
        jnp.bfloat16
    )
    capacity = 3 * count * TOP // (2 * experts)
    flat_ids = (route_group[:, None] * per_group + route_expert).reshape(-1)
    columns = lax.broadcasted_iota(jnp.int32, (flat_ids.shape[0], experts), 1)
    onehot = (flat_ids[:, None] == columns).astype(jnp.int32)
    rank = jnp.sum((jnp.cumsum(onehot, axis=0) - 1) * onehot, axis=1)
    dump = experts * capacity
    slot = jnp.where(rank < capacity, flat_ids * capacity + rank, dump)
    rows = jnp.repeat(normed, TOP, axis=0)
    outgoing = (
        jnp.zeros((dump + 1, width), jnp.bfloat16)
        .at[slot]
        .set(rows)[:-1]
        .reshape(experts, capacity, width)
    )
    block = lax.all_to_all(outgoing, ("fs", "tp"), split_axis=0, concat_axis=0, tiled=True)
    flat_rows = block.reshape(-1, width)
    gate = jnp.dot(flat_rows, gate_new[0], preferred_element_type=jnp.float32)
    upper = jnp.dot(flat_rows, up_new[0], preferred_element_type=jnp.float32)
    hidden = (jax.nn.silu(gate) * upper).astype(jnp.bfloat16)
    result = jnp.dot(hidden, down_new[0], preferred_element_type=jnp.float32).astype(jnp.bfloat16)
    outcome = result.reshape(block.shape)
    returned = lax.all_to_all(outcome, ("fs", "tp"), split_axis=0, concat_axis=0, tiled=True)
    table = jnp.concatenate(
        [returned.reshape(-1, width), jnp.zeros((1, width), jnp.bfloat16)], axis=0
    )
    picked = table[slot].reshape(count, TOP, width).astype(jnp.float32)
    mixed = jnp.sum(picked * route_weight[:, :, None], axis=1).astype(jnp.bfloat16)
    return (gate_new, up_new, down_new, mixed)


def solution(mesh):
    placed = (
        P(("gr", "fs", "tp"), None),
        P("fs"),
        P(None, "fs", ("gr", "tp")),
        P(None, "fs", ("gr", "tp")),
        P(None, "fs", ("gr", "tp")),
        P(("gr", "fs", "tp")),
        P(("gr", "fs", "tp"), None),
        P(("gr", "fs", "tp"), None),
    )

    def body(*args):
        n = mesh.shape["fs"] * mesh.shape["tp"]
        cap = 3 * args[0].shape[0] * TOP // (2 * n)
        small = n <= 16 and n & (n - 1) == 0 and cap % 8 == 0 and mesh.shape["gr"] == 2
        if not small:
            return slow_body(*args)
        return fast_body(*args)

    return jax.shard_map(
        body,
        mesh=mesh,
        in_specs=placed,
        out_specs=(
            P(("fs", "tp"), None, None),
            P(("fs", "tp"), None, None),
            P(("fs", "tp"), None, None),
            P(("gr", "fs", "tp"), None),
        ),
        check_vma=False,
    )
```
